32 devices in a mesh: ep: 4 (over y, x), tp: 8 (over z, core).
Axes of the slice: x: 2, y: 2, z: 4, core: 2. Of those that a mesh axis runs over, the one named last changes fastest.
Arguments:
- queries: bfloat16 [4096, 1024], P('ep', 'tp'), may hold values from -600 to 600
- key_rows: bfloat16 [4096, 128], P('ep'), may hold values from -6 to 6
- value_rows: bfloat16 [4096, 128], P('ep'), may hold values from -48 to 48
- sink_logits: float32 [16], P('tp'), may hold values from 2 to 6
- out_weight: bfloat16 [1024, 2048], P('tp'), may hold values from -0.1875 to 0.1875
- moe_rows: bfloat16 [1024, 2048], P(('ep', 'tp')), may hold values from -6 to 6
- moe_gain: float32 [2048], replicated, may hold values from 0.1 to 1.9
- routes: int32 [1024, 2], P(('ep', 'tp')), may hold values from 0 to 3, all different within a row; in each aligned block of 32 rows (0 to 31, 32 to 63, ...) at most 24 rows name the same one
- route_weight: float32 [1024, 2], P(('ep', 'tp')), may hold values from 0.2 to 1
- gate_weight: bfloat16 [4, 2048, 7168], P('ep', None, 'tp'), may hold values from -0.125 to 0.125
- up_weight: bfloat16 [4, 2048, 7168], P('ep', None, 'tp'), may hold values from -0.125 to 0.125
- down_weight: bfloat16 [4, 7168, 2048], P('ep', 'tp'), may hold values from -0.0625 to 0.0625
Outputs:
- mixer_out: bfloat16 [4096, 2048], P(('ep', 'tp'))
- moe_out: bfloat16 [1024, 2048], P(('ep', 'tp'))
The draws below stay inside these ranges and needn't reach their ends.
Inputs may be any that keep to these rules, and one draw needn't show every extreme that they name: `routes`: in each aligned block of 32 rows (the rows of one device) no expert is named more than 24 times, a bound that some block reaches; each row names 2 different experts.
All inputs are finite; a program needn't handle non-finite values.
Results may differ from the reference program's by a relative error of at most 0.02.
Values may be sent and summed in bfloat16 or wider, within the bound.
A program may use at most 128 MiB of HBM per device.

```python
import math
import jax
import jax.numpy as jnp
import numpy as np
from jax import lax

D = 2048
HEADS = 16
KV_HEADS = 2
HEAD_DIM = 64
WINDOW = 128
FF = 7168
TOP = 2
MOE_DEV = 32
EXPERTS = 4
TOKENS = 4096
MOE_TOKENS = 1024
CAP = 24
N_TP = 8


def draw_queries(key, part):
    base = jax.random.truncated_normal(key, -6.0, 6.0, (TOKENS, HEADS * HEAD_DIM), jnp.float32)
    return base.astype(jnp.bfloat16)


def block_levels(rng, extent, shards, smallest, largest):
    level, own = 1.0, jax.random.fold_in(rng, 6)
    for dim, shards_of in shards:
        draws = jnp.exp(jax.random.uniform(jax.random.fold_in(own, dim), (shards_of,), jnp.float32, smallest / len(shards), largest / len(shards)))
        level = level * jnp.repeat(draws, extent[dim] // shards_of).reshape([-1 if axis == dim else 1 for axis in range(len(extent))])
    return level


def assign_block(own_key, own, number, rows, count, top, most, slope):
    sequence = jax.random.permutation(own_key, count)
    crowded, ordinary = portions_of(count, rows * top, most, slope, True), portions_of(count, rows * top, most, slope, False)
    places = jnp.arange(count)

    def named(tallies, turn):
        used = int((tallies > 0).sum())
        fixed = max(1, used // 4)
        shifted = fixed + (places - fixed + turn * (used - fixed)) % max(1, count - fixed)
        return jnp.zeros((count,), jnp.int32).at[sequence[jnp.where(places < fixed, places, shifted)]].set(jnp.asarray(tallies, jnp.int32))

    tallies = jnp.where(number % 4 == 0, named(crowded, number // 4), named(ordinary, number - number // 4 - 1))
    mixed = jax.random.permutation(jax.random.fold_in(own, 3), count)
    donor, receiver = mixed[0:count // 2 * 2:2], mixed[1:count // 2 * 2:2]
    room = jnp.minimum(tallies[donor] - 1, most - tallies[receiver]) // 2
    room = jnp.where((donor == sequence[0]) | (receiver == sequence[0]) | (tallies[receiver] == 0), 0, jnp.maximum(room, 0))
    shifted = jax.random.randint(jax.random.fold_in(own, 4), (count // 2,), 0, 1 << 20) % (room + 1)
    tallies = tallies.at[donor].add(-shifted).at[receiver].add(shifted)
    members = jnp.searchsorted(jnp.cumsum(tallies), jnp.arange(rows * top), side="right").astype(jnp.int32)
    listing = members.reshape(top, rows).T
    listing = listing[jax.random.permutation(jax.random.fold_in(own, 1), rows)]
    turn = jax.random.randint(jax.random.fold_in(own, 2), (rows, 1), 0, top)
    return jnp.take_along_axis(listing, (jnp.arange(top)[None, :] + turn) % top, axis=1)


def portions_of(amount, total, most, slope, full):
    loads = [(1 << 20) // math.isqrt(standing ** slope) + 1 for standing in range(1, amount + 1)]
    largest = most if full else min(most, max(-(-total // amount), total * loads[0] // sum(loads)))
    least = 1 if total - largest >= amount - 1 else 0
    given, rest = [largest] + [least] * (amount - 1), total - largest - least * (amount - 1)
    while rest > 0:
        free = [i for i in range(1, amount) if given[i] < largest] or [i for i in range(1, amount) if given[i] < most]
        mass, budget = sum([loads[i] for i in free]), rest
        for i in free:
            more = min(most - given[i], max(1, budget * loads[i] // mass), rest)
            given[i] = given[i] + more
            rest = rest - more
    return np.array(given)


def centred(rng, dims, scale, bound, shards=(), kind=jnp.bfloat16):
    level = block_levels(rng, dims, shards, -0.22, 0.18) if shards else 1.0
    drawn = jax.random.normal(rng, dims, jnp.float32) * scale * level
    return jnp.minimum(jnp.maximum(drawn, -bound), bound).astype(kind)


def setup_inputs(seed: int = 0) -> dict:
    seeds = jax.random.split(jax.random.key(seed), 13)
    queries = draw_queries(jax.random.fold_in(seeds[12], 71), 0)
    key_rows = centred(seeds[1], (TOKENS, KV_HEADS * HEAD_DIM), 1.0, 6.0, ((0, 4),))
    value_rows = centred(seeds[2], (TOKENS, KV_HEADS * HEAD_DIM), 8.0, 48.0, ((0, 4),))
    sink_logits = jnp.clip(2.0 + 4.0 * jax.random.uniform(seeds[3], (HEADS,), jnp.float32) ** block_levels(seeds[3], (HEADS,), ((0, 8),), -0.2, 0.2), 2.0, 6.0)
    out_weight = centred(seeds[4], (HEADS * HEAD_DIM, D), (HEADS * HEAD_DIM) ** -0.5, 0.1875, ((0, 8),))
    moe_rows = centred(seeds[5], (MOE_TOKENS, D), 1.0, 6.0, ((0, 32),))
    moe_gain = jnp.clip(1.0 + 0.18 * jax.random.normal(seeds[6], (D,), jnp.float32), 0.1, 1.9)
    routes_keys = jax.random.split(jax.random.fold_in(seeds[7], 1), MOE_TOKENS // MOE_DEV)
    routes_turns = jax.random.permutation(jax.random.fold_in(seeds[7], 3), MOE_TOKENS // MOE_DEV)
    routes = jax.vmap(lambda own, number: assign_block(jax.random.fold_in(seeds[7], 2), own, number, MOE_DEV, EXPERTS, TOP, CAP, 2))(routes_keys, routes_turns).reshape((MOE_TOKENS, TOP))
    route_weight = jnp.clip(0.2 + 0.8 * jax.random.uniform(seeds[8], (MOE_TOKENS, TOP), jnp.float32) ** block_levels(seeds[8], (MOE_TOKENS, TOP), ((0, 32),), -0.2, 0.2), 0.2, 1.0)
    gate_weight = centred(seeds[9], (EXPERTS, D, FF), D ** -0.5, 0.125, ((0, 4), (2, 8)))
    up_weight = centred(seeds[10], (EXPERTS, D, FF), D ** -0.5, 0.125, ((0, 4), (2, 8)))
    down_weight = centred(seeds[11], (EXPERTS, FF, D), FF ** -0.5, 0.0625, ((0, 4), (1, 8)))
    return {"queries": queries, "key_rows": key_rows, "value_rows": value_rows, "sink_logits": sink_logits, "out_weight": out_weight, "moe_rows": moe_rows, "moe_gain": moe_gain, "routes": routes, "route_weight": route_weight, "gate_weight": gate_weight, "up_weight": up_weight, "down_weight": down_weight}


big_negative = -1e+30
norm_eps = 1e-05

def stored_bf16(values):
    return lax.optimization_barrier(values.astype(jnp.bfloat16)).astype(jnp.float32)

def layer_normed(inputs, gain):
    values = inputs.astype(jnp.float32)
    center = values - lax.optimization_barrier(jnp.mean(values, -1, keepdims=True))
    spread = lax.optimization_barrier(jnp.mean(center * center, -1, keepdims=True))
    return (center * lax.rsqrt(spread + norm_eps) * gain).astype(jnp.bfloat16)

def one_head(head_index, queries, key_rows, value_rows, sink_logits):
    total = queries.shape[0]
    blocks = total // WINDOW
    key_head = head_index // (HEADS // KV_HEADS)
    query_cols = lax.dynamic_slice_in_dim(queries, head_index * HEAD_DIM, HEAD_DIM, 1).astype(jnp.float32)
    key_cols = lax.dynamic_slice_in_dim(key_rows, key_head * HEAD_DIM, HEAD_DIM, 1).astype(jnp.float32)
    value_cols = lax.dynamic_slice_in_dim(value_rows, key_head * HEAD_DIM, HEAD_DIM, 1).astype(jnp.float32)
    padding = jnp.zeros((WINDOW, HEAD_DIM), jnp.float32)
    key_ext = jnp.concatenate([padding, key_cols], 0)
    value_ext = jnp.concatenate([padding, value_cols], 0)
    key_blocks = jnp.concatenate([key_ext[:total].reshape(blocks, WINDOW, HEAD_DIM), key_ext[WINDOW:].reshape(blocks, WINDOW, HEAD_DIM)], 1)
    value_blocks = jnp.concatenate([value_ext[:total].reshape(blocks, WINDOW, HEAD_DIM), value_ext[WINDOW:].reshape(blocks, WINDOW, HEAD_DIM)], 1)
    scores = jnp.einsum('nqd,nkd->nqk', query_cols.reshape(blocks, WINDOW, HEAD_DIM), key_blocks) * HEAD_DIM ** (-0.5)
    block_base = jnp.arange(blocks, dtype=jnp.int32)[:, None, None] * WINDOW
    query_pos = block_base + jnp.arange(WINDOW, dtype=jnp.int32)[None, :, None]
    key_pos = block_base - WINDOW + jnp.arange(2 * WINDOW, dtype=jnp.int32)[None, None, :]
    allowed = (key_pos <= query_pos) & (key_pos > query_pos - WINDOW) & (key_pos >= 0)
    masked = jnp.where(allowed, scores, big_negative)
    sink = sink_logits[head_index]
    row_max = jnp.maximum(lax.optimization_barrier(jnp.max(masked, -1)), sink)
    powers = jnp.where(allowed, jnp.exp(masked - row_max[..., None]), 0.0)
    totals = lax.optimization_barrier(jnp.sum(powers, -1)) + jnp.exp(sink - row_max)
    attn_probs = stored_bf16(powers / totals[..., None])
    attended = jnp.einsum('nqk,nkd->nqd', attn_probs, value_blocks)
    return attended.astype(jnp.bfloat16).reshape(total, HEAD_DIM)

def one_expert(inputs):
    expert_rows, gate_mat, up_mat, down_mat = inputs
    gate_val = jnp.dot(expert_rows, gate_mat, preferred_element_type=jnp.float32)
    up_val = jnp.dot(expert_rows, up_mat, preferred_element_type=jnp.float32)
    hidden = (jax.nn.silu(gate_val) * up_val).astype(jnp.bfloat16)
    group_units = FF // N_TP

    def add_group(index, carry):
        first_col = index.astype(jnp.int32) * group_units
        hidden_cols = lax.dynamic_slice_in_dim(hidden, first_col, group_units, 1)
        down_rows = lax.dynamic_slice_in_dim(down_mat, first_col, group_units, 0)
        return carry + stored_bf16(jnp.dot(hidden_cols, down_rows, preferred_element_type=jnp.float32))
    summed = lax.fori_loop(0, N_TP, add_group, jnp.zeros((expert_rows.shape[0], D), jnp.float32))
    return summed.astype(jnp.bfloat16)

def reference(queries, key_rows, value_rows, sink_logits, out_weight, moe_rows, moe_gain, routes, route_weight, gate_weight, up_weight, down_weight):
    total = queries.shape[0]
    per_head = lax.map(lambda index: one_head(index, queries, key_rows, value_rows, sink_logits), jnp.arange(HEADS, dtype=jnp.int32))
    attended = jnp.transpose(per_head, (1, 0, 2)).reshape(total, HEADS * HEAD_DIM)
    group_cols = HEADS // N_TP * HEAD_DIM

    def add_heads(index, carry):
        first_col = index.astype(jnp.int32) * group_cols
        head_cols = lax.dynamic_slice_in_dim(attended, first_col, group_cols, 1)
        proj_rows = lax.dynamic_slice_in_dim(out_weight, first_col, group_cols, 0)
        return carry + stored_bf16(jnp.dot(head_cols, proj_rows, preferred_element_type=jnp.float32))
    mixer_out = lax.fori_loop(0, N_TP, add_heads, jnp.zeros((total, D), jnp.float32)).astype(jnp.bfloat16)
    normed = layer_normed(moe_rows, moe_gain)
    devices = MOE_TOKENS // MOE_DEV
    chosen = routes.reshape(devices, MOE_DEV * TOP).astype(jnp.int32)
    onehot = (chosen[..., None] == jnp.arange(EXPERTS, dtype=jnp.int32)[None, None, :]).astype(jnp.int32)
    earlier_count = jnp.cumsum(onehot, 1) - onehot
    slot_index = lax.optimization_barrier(jnp.sum(earlier_count * onehot, -1)).astype(jnp.int32)
    device_index = jnp.arange(devices, dtype=jnp.int32)[:, None]
    position = ((chosen * devices + device_index) * CAP + slot_index).reshape(-1).astype(jnp.int32)
    token_of = (jnp.arange(MOE_TOKENS * TOP, dtype=jnp.int32) // TOP).astype(jnp.int32)
    buffer = jnp.zeros((EXPERTS * devices * CAP, D), jnp.bfloat16).at[position].set(normed[token_of])
    buffer = buffer.reshape(EXPERTS, devices * CAP, D)
    results = lax.map(one_expert, (buffer, gate_weight, up_weight, down_weight))
    picked = results.reshape(EXPERTS * devices * CAP, D)[position].astype(jnp.float32)
    picked = picked.reshape(MOE_TOKENS, TOP, D)
    moe_out = lax.optimization_barrier(jnp.sum(picked * route_weight[:, :, None], 1)).astype(jnp.bfloat16)
    return (mixer_out, moe_out)
```

```python
import jax
import jax.numpy as jnp
from jax import lax
from jax.sharding import PartitionSpec as P

HEADS = 16
KV_HEADS = 2
HEAD_DIM = 64
WINDOW = 128
TOP = 2


big_negative = -1e30
norm_eps = 1e-05


def passed_along(value, axis, steps):
    count = lax.axis_size(axis)
    initial, last = (max(0, -steps), min(count, count - steps))
    return lax.ppermute(value, axis, [(source, source + steps) for source in range(initial, last)])


def layer_normed(inputs, gain):
    values = inputs.astype(jnp.float32)
    center = values - jnp.mean(values, -1, keepdims=True)
    spread = jnp.mean(center * center, -1, keepdims=True)
    return (center * lax.rsqrt(spread + norm_eps) * gain).astype(jnp.bfloat16)


def attend(queries, key_rows, value_rows, sink_logits):
    total = queries.shape[0]
    heads_here = sink_logits.shape[0]
    blocks = total // WINDOW
    key_head = lax.axis_index("tp") * heads_here // (HEADS // KV_HEADS)
    key_own = lax.dynamic_slice_in_dim(key_rows, key_head * HEAD_DIM, HEAD_DIM, 1)
    value_own = lax.dynamic_slice_in_dim(value_rows, key_head * HEAD_DIM, HEAD_DIM, 1)
    last_rows = jnp.concatenate([key_own[total - WINDOW :], value_own[total - WINDOW :]], 1)
    earlier = passed_along(last_rows, "ep", 1)
    key_ext = jnp.concatenate([earlier[:, :HEAD_DIM], key_own], 0)
    value_ext = jnp.concatenate([earlier[:, HEAD_DIM:], value_own], 0)
    key_blocks = jnp.concatenate(
        [
            key_ext[:total].reshape(blocks, WINDOW, HEAD_DIM),
            key_ext[WINDOW:].reshape(blocks, WINDOW, HEAD_DIM),
        ],
        1,
    )
    value_blocks = jnp.concatenate(
        [
            value_ext[:total].reshape(blocks, WINDOW, HEAD_DIM),
            value_ext[WINDOW:].reshape(blocks, WINDOW, HEAD_DIM),
        ],
        1,
    )
    query_blocks = queries.reshape(blocks, WINDOW, heads_here, HEAD_DIM)
    scores = jnp.einsum(
        "nqhd,nkd->nhqk", query_blocks, key_blocks, preferred_element_type=jnp.float32
    ) * HEAD_DIM ** (-0.5)
    anchor = lax.axis_index("ep") * total
    block_base = anchor + jnp.arange(blocks, dtype=jnp.int32)[:, None, None] * WINDOW
    query_pos = block_base + jnp.arange(WINDOW, dtype=jnp.int32)[None, :, None]
    key_pos = block_base - WINDOW + jnp.arange(2 * WINDOW, dtype=jnp.int32)[None, None, :]
    allowed = ((key_pos <= query_pos) & (key_pos > query_pos - WINDOW) & (key_pos >= 0))[:, None]
    masked = jnp.where(allowed, scores, big_negative)
    sinks = sink_logits[None, :, None]
    row_max = jnp.maximum(jnp.max(masked, -1), sinks)
    powers = jnp.where(allowed, jnp.exp(masked - row_max[..., None]), 0.0)
    totals = jnp.sum(powers, -1) + jnp.exp(sinks - row_max)
    attn_probs = (powers / totals[..., None]).astype(jnp.bfloat16)
    attended = jnp.einsum(
        "nhqk,nkd->nqhd", attn_probs, value_blocks, preferred_element_type=jnp.float32
    )
    return attended.astype(jnp.bfloat16).reshape(total, heads_here * HEAD_DIM)


def mixer(queries, key_rows, value_rows, sink_logits, out_weight):
    attended = attend(queries, key_rows, value_rows, sink_logits)
    return lax.psum_scatter(
        jnp.dot(attended, out_weight, preferred_element_type=jnp.float32).astype(jnp.bfloat16),
        "tp",
        scatter_dimension=0,
        tiled=True,
    )


def experts(moe_rows, moe_gain, routes, route_weight, gate_weight, up_weight, down_weight):
    row_count = moe_rows.shape[0]
    width_all = moe_rows.shape[1]
    expert_count = gate_weight.shape[0] * lax.axis_size("ep")
    capacity = 3 * row_count * TOP // (2 * expert_count)
    normed = layer_normed(moe_rows, moe_gain)
    chosen = routes.reshape(-1)
    onehot = (chosen[:, None] == jnp.arange(expert_count, dtype=jnp.int32)[None, :]).astype(
        jnp.int32
    )
    earlier_count = jnp.cumsum(onehot, 0) - onehot
    slot_index = jnp.sum(earlier_count * onehot, 1)
    target = chosen * capacity + slot_index
    matches = target[None, :] == jnp.arange(expert_count * capacity, dtype=jnp.int32)[:, None]
    dispatch_map = jnp.sum(matches.reshape(expert_count * capacity, row_count, TOP), -1).astype(
        jnp.bfloat16
    )
    buffer = jnp.dot(dispatch_map, normed, preferred_element_type=jnp.float32).astype(jnp.bfloat16)
    buffer = buffer.reshape(expert_count, capacity, width_all)
    gate_mat = gate_weight[0]
    up_mat = up_weight[0]
    down_mat = down_weight[0]
    received = lax.all_to_all(buffer, "ep", split_axis=0, concat_axis=0, tiled=True)
    total = received.shape[0] * received.shape[1]
    flat_rows = received.reshape(total, width_all)
    shard_rows = lax.all_gather(flat_rows, "tp", axis=0, tiled=True)
    gate_val = jnp.dot(shard_rows, gate_mat, preferred_element_type=jnp.float32)
    up_val = jnp.dot(shard_rows, up_mat, preferred_element_type=jnp.float32)
    hidden = (jax.nn.silu(gate_val) * up_val).astype(jnp.bfloat16)
    summed = lax.psum_scatter(
        jnp.dot(hidden, down_mat, preferred_element_type=jnp.float32).astype(jnp.bfloat16),
        "tp",
        scatter_dimension=0,
        tiled=True,
    )
    results = summed.reshape(received.shape)
    returned = lax.all_to_all(results, "ep", split_axis=0, concat_axis=0, tiled=True)
    weights_flat = route_weight.reshape(-1)
    combine_map = jnp.sum(
        jnp.where(matches, weights_flat[None, :], 0.0).reshape(
            expert_count * capacity, row_count, TOP
        ),
        -1,
    )
    returned_flat = returned.reshape(expert_count * capacity, width_all).astype(jnp.float32)
    moe_out = lax.dot_general(
        combine_map, returned_flat, (((0,), (0,)), ((), ())), precision=lax.Precision.HIGHEST
    )
    return moe_out.astype(jnp.bfloat16)


def dense_experts(moe_rows, moe_gain, routes, route_weight, gate_weight, up_weight, down_weight):
    count = lax.axis_size("ep")
    normed = layer_normed(moe_rows, moe_gain)
    both = ("ep", "tp")
    rows = lax.all_gather(normed, both, axis=0, tiled=True)
    named = routes[:, :, None] == jnp.arange(count, dtype=jnp.int32)[None, None, :]
    shares = jnp.sum(jnp.where(named, route_weight[:, :, None], 0.0), 1)
    shares = lax.all_gather(shares, both, axis=0, tiled=True)
    share = lax.dynamic_slice_in_dim(shares, lax.axis_index("ep"), 1, 1)
    gate_val = jnp.dot(rows, gate_weight[0], preferred_element_type=jnp.float32)
    up_val = jnp.dot(rows, up_weight[0], preferred_element_type=jnp.float32)
    hidden = (jax.nn.silu(gate_val) * up_val).astype(jnp.bfloat16)
    down = jnp.dot(hidden, down_weight[0], preferred_element_type=jnp.float32)
    return lax.psum_scatter(
        (down * share).astype(jnp.bfloat16), both, scatter_dimension=0, tiled=True
    )


def body(
    queries,
    key_rows,
    value_rows,
    sink_logits,
    out_weight,
    moe_rows,
    moe_gain,
    routes,
    route_weight,
    gate_weight,
    up_weight,
    down_weight,
):
    mixer_out = mixer(queries, key_rows, value_rows, sink_logits, out_weight)
    slots = 3 * moe_rows.shape[0] * TOP // 2
    sparse = slots * lax.axis_size("tp") < moe_rows.shape[0] * lax.axis_size("tp") * lax.axis_size("ep") // 2
    layer = experts if sparse else dense_experts
    moe_out = layer(moe_rows, moe_gain, routes, route_weight, gate_weight, up_weight, down_weight)
    return (mixer_out, moe_out)


def solution(mesh):
    in_specs = (
        P("ep", "tp"),
        P("ep", None),
        P("ep", None),
        P("tp"),
        P("tp", None),
        P(("ep", "tp"), None),
        P(),
        P(("ep", "tp"), None),
        P(("ep", "tp"), None),
        P("ep", None, "tp"),
        P("ep", None, "tp"),
        P("ep", "tp", None),
    )
    out_specs = (P(("ep", "tp"), None), P(("ep", "tp"), None))
    return jax.shard_map(body, mesh=mesh, in_specs=in_specs, out_specs=out_specs, check_vma=False)
```

```python
import functools

import jax
import jax.numpy as jnp
from jax import lax
from jax.experimental import pallas as pl
from jax.experimental.pallas import tpu as pltpu
from jax.sharding import PartitionSpec as P

MESH = pl.DeviceIdType.MESH

HEADS = 16
KV_HEADS = 2
HEAD_DIM = 64
WINDOW = 128
TOP = 2


big_negative = -1e30
norm_eps = 1e-05


def passed_along(value, axis, steps):
    count = lax.axis_size(axis)
    initial, last = (max(0, -steps), min(count, count - steps))
    return lax.ppermute(value, axis, [(source, source + steps) for source in range(initial, last)])


def layer_normed(inputs, gain):
    values = inputs.astype(jnp.float32)
    center = values - jnp.mean(values, -1, keepdims=True)
    spread = jnp.mean(center * center, -1, keepdims=True)
    return (center * lax.rsqrt(spread + norm_eps) * gain).astype(jnp.bfloat16)


def attend(queries, key_rows, value_rows, sink_logits):
    total = queries.shape[0]
    heads_here = sink_logits.shape[0]
    blocks = total // WINDOW
    key_head = lax.axis_index("tp") * heads_here // (HEADS // KV_HEADS)
    key_own = lax.dynamic_slice_in_dim(key_rows, key_head * HEAD_DIM, HEAD_DIM, 1)
    value_own = lax.dynamic_slice_in_dim(value_rows, key_head * HEAD_DIM, HEAD_DIM, 1)
    last_rows = jnp.concatenate([key_own[total - WINDOW :], value_own[total - WINDOW :]], 1)
    earlier = passed_along(last_rows, "ep", 1)
    key_ext = jnp.concatenate([earlier[:, :HEAD_DIM], key_own], 0)
    value_ext = jnp.concatenate([earlier[:, HEAD_DIM:], value_own], 0)
    key_blocks = jnp.concatenate(
        [
            key_ext[:total].reshape(blocks, WINDOW, HEAD_DIM),
            key_ext[WINDOW:].reshape(blocks, WINDOW, HEAD_DIM),
        ],
        1,
    )
    value_blocks = jnp.concatenate(
        [
            value_ext[:total].reshape(blocks, WINDOW, HEAD_DIM),
            value_ext[WINDOW:].reshape(blocks, WINDOW, HEAD_DIM),
        ],
        1,
    )
    query_blocks = queries.reshape(blocks, WINDOW, heads_here, HEAD_DIM)
    scores = jnp.einsum(
        "nqhd,nkd->nhqk", query_blocks, key_blocks, preferred_element_type=jnp.float32
    ) * HEAD_DIM ** (-0.5)
    anchor = lax.axis_index("ep") * total
    block_base = anchor + jnp.arange(blocks, dtype=jnp.int32)[:, None, None] * WINDOW
    query_pos = block_base + jnp.arange(WINDOW, dtype=jnp.int32)[None, :, None]
    key_pos = block_base - WINDOW + jnp.arange(2 * WINDOW, dtype=jnp.int32)[None, None, :]
    allowed = ((key_pos <= query_pos) & (key_pos > query_pos - WINDOW) & (key_pos >= 0))[:, None]
    masked = jnp.where(allowed, scores, big_negative)
    sinks = sink_logits[None, :, None]
    row_max = jnp.maximum(jnp.max(masked, -1), sinks)
    powers = jnp.where(allowed, jnp.exp(masked - row_max[..., None]), 0.0)
    totals = jnp.sum(powers, -1) + jnp.exp(sinks - row_max)
    attn_probs = (powers / totals[..., None]).astype(jnp.bfloat16)
    attended = jnp.einsum(
        "nhqk,nkd->nqhd", attn_probs, value_blocks, preferred_element_type=jnp.float32
    )
    return attended.astype(jnp.bfloat16).reshape(total, heads_here * HEAD_DIM)


def mixer(queries, key_rows, value_rows, sink_logits, out_weight):
    attended = attend(queries, key_rows, value_rows, sink_logits)
    return lax.psum_scatter(
        jnp.dot(attended, out_weight, preferred_element_type=jnp.float32).astype(jnp.bfloat16),
        "tp",
        scatter_dimension=0,
        tiled=True,
    )


def experts(moe_rows, moe_gain, routes, route_weight, gate_weight, up_weight, down_weight):
    row_count = moe_rows.shape[0]
    width_all = moe_rows.shape[1]
    expert_count = gate_weight.shape[0] * lax.axis_size("ep")
    capacity = 3 * row_count * TOP // (2 * expert_count)
    normed = layer_normed(moe_rows, moe_gain)
    chosen = routes.reshape(-1)
    onehot = (chosen[:, None] == jnp.arange(expert_count, dtype=jnp.int32)[None, :]).astype(
        jnp.int32
    )
    earlier_count = jnp.cumsum(onehot, 0) - onehot
    slot_index = jnp.sum(earlier_count * onehot, 1)
    target = chosen * capacity + slot_index
    matches = target[None, :] == jnp.arange(expert_count * capacity, dtype=jnp.int32)[:, None]
    dispatch_map = jnp.sum(matches.reshape(expert_count * capacity, row_count, TOP), -1).astype(
        jnp.bfloat16
    )
    buffer = jnp.dot(dispatch_map, normed, preferred_element_type=jnp.float32).astype(jnp.bfloat16)
    buffer = buffer.reshape(expert_count, capacity, width_all)
    gate_mat = gate_weight[0]
    up_mat = up_weight[0]
    down_mat = down_weight[0]
    received = lax.all_to_all(buffer, "ep", split_axis=0, concat_axis=0, tiled=True)
    total = received.shape[0] * received.shape[1]
    flat_rows = received.reshape(total, width_all)
    shard_rows = lax.all_gather(flat_rows, "tp", axis=0, tiled=True)
    gate_val = jnp.dot(shard_rows, gate_mat, preferred_element_type=jnp.float32)
    up_val = jnp.dot(shard_rows, up_mat, preferred_element_type=jnp.float32)
    hidden = (jax.nn.silu(gate_val) * up_val).astype(jnp.bfloat16)
    summed = lax.psum_scatter(
        jnp.dot(hidden, down_mat, preferred_element_type=jnp.float32).astype(jnp.bfloat16),
        "tp",
        scatter_dimension=0,
        tiled=True,
    )
    results = summed.reshape(received.shape)
    returned = lax.all_to_all(results, "ep", split_axis=0, concat_axis=0, tiled=True)
    weights_flat = route_weight.reshape(-1)
    combine_map = jnp.sum(
        jnp.where(matches, weights_flat[None, :], 0.0).reshape(
            expert_count * capacity, row_count, TOP
        ),
        -1,
    )
    returned_flat = returned.reshape(expert_count * capacity, width_all).astype(jnp.float32)
    moe_out = lax.dot_general(
        combine_map, returned_flat, (((0,), (0,)), ((), ())), precision=lax.Precision.HIGHEST
    )
    return moe_out.astype(jnp.bfloat16)


def fused_kernel(
    groups,
    ranks,
    q_ref,
    key_ref,
    value_ref,
    tile_ref,
    rows_ref,
    gain_ref,
    ow_hbm,
    gate_hbm,
    up_hbm,
    down_hbm,
    mix_ref,
    moe_ref,
    x_buf,
    p_buf,
    r1_buf,
    r2_buf,
    r3_buf,
    ru_buf,
    rd_buf,
    w_buf,
    qb_buf,
    tiles,
    halo,
    kdup,
    vdup,
    att,
    gate_w,
    up_w,
    down_w,
    load_sem,
    tile_ss,
    tile_rs,
    q_ss,
    q_rs,
    halo_ss,
    halo_rs,
    up_ss,
    up_rs,
    dn_ss,
    dn_rs,
    pa_ss,
    pa_rs,
    x1_ss,
    x1_rs,
    x2_ss,
    x2_rs,
    wu_ss,
    wu_rs,
    wd_ss,
    wd_rs,
    wp_ss,
    wp_rs,
    s1_ss,
    s1_rs,
    s2_ss,
    s2_rs,
    s3_ss,
    s3_rs,
    ru_ss,
    ru_rs,
    rd_ss,
    rd_rs,
):
    chips = ranks // 2
    total = groups * ranks
    e, t = lax.axis_index("ep"), lax.axis_index("tp")
    z, c = lax.div(t, 2), lax.rem(t, 2)
    y, x = lax.div(e, 2), lax.rem(e, 2)
    me = e * ranks + t
    ex, ey, e3 = e + 1 - 2 * x, e + 2 - 4 * y, 3 - e
    e1 = ex * (1 - c) + ey * c
    e2 = ey * (1 - c) + ex * c
    other = t + 1 - 2 * c
    oc = 1 - c
    columns = (e, e1, e2, e3)
    pending = []

    def remote(src, dst, ss, rs, to):
        return pltpu.make_async_remote_copy(
            src_ref=src, dst_ref=dst, send_sem=ss, recv_sem=rs, device_id=to, device_id_type=MESH
        )

    def send(src, dst, ss, rs, to, when=None):
        copy = remote(src, dst, ss, rs, to)
        pending.append((when, copy))
        if when is None:
            copy.start()
        else:
            pl.when(when)(copy.start)

    def received(dst, ss, rs):
        remote(dst, dst, ss, rs, (e, other)).wait_recv()

    loads = [
        pltpu.make_async_copy(ow_hbm, w_buf.at[t], load_sem.at[0]),
        pltpu.make_async_copy(gate_hbm.at[0], gate_w, load_sem.at[1]),
        pltpu.make_async_copy(up_hbm.at[0], up_w, load_sem.at[2]),
        pltpu.make_async_copy(down_hbm.at[0], down_w, load_sem.at[3]),
    ]
    for load in loads:
        load.start()

    barrier = pltpu.get_barrier_semaphore()

    @pl.loop(1, total)
    def _(j):
        to = lax.rem(me + j, total)
        pl.semaphore_signal(
            barrier,
            inc=1,
            device_id=(lax.div(to, ranks), lax.rem(to, ranks)),
            device_id_type=MESH,
        )

    values = rows_ref[...].astype(jnp.float32)
    center = values - jnp.mean(values, -1, keepdims=True)
    spread = jnp.mean(center * center, -1, keepdims=True)
    x_buf[e, z, c] = (center * lax.rsqrt(spread + norm_eps) * gain_ref[...]).astype(jnp.bfloat16)
    tiles[me] = tile_ref[...]
    qb_buf[t] = q_ref[pl.ds(pl.multiple_of(t * WINDOW, WINDOW), WINDOW), :]

    pl.semaphore_wait(barrier, total - 1)

    def spread_block(zz, up, down, when):
        block = x_buf.at[e, zz, c]
        if up:
            ok = z < chips - 1
            ok = ok if when is None else ok & when
            send(block, block, up_ss.at[zz], up_rs.at[zz], (e, t + 2), ok)
        if down:
            ok = z > 0
            ok = ok if when is None else ok & when
            send(block, block, dn_ss.at[zz], dn_rs.at[zz], (e, t - 2), ok)
        send(block, block, x1_ss.at[zz], x1_rs.at[zz], (e1, t), when)
        send(block, block, x2_ss.at[zz], x2_rs.at[zz], (e2, t), when)
        send(block, block, pa_ss.at[zz], pa_rs.at[zz], (e, other), when)

    spread_block(z, True, True, None)

    @pl.loop(1, ranks)
    def _(j):
        tt = lax.rem(t + j, ranks)
        remote(
            q_ref.at[pl.ds(pl.multiple_of(tt * WINDOW, WINDOW), WINDOW), :],
            qb_buf.at[t],
            q_ss.at[j],
            q_rs.at[j],
            (e, tt),
        ).start()

    @pl.loop(1, total)
    def _(j):
        to = lax.rem(me + j, total)
        remote(
            tile_ref,
            tiles.at[me],
            tile_ss.at[j],
            tile_rs.at[j],
            (lax.div(to, ranks), lax.rem(to, ranks)),
        ).start()

    last = key_ref.shape[0] - WINDOW
    gives = (t == 0) & (e < groups - 1)
    takes = (t == 0) & (e > 0)
    for i, source in enumerate((key_ref, value_ref)):
        send(
            source.at[pl.ds(last, WINDOW), :],
            halo.at[i],
            halo_ss.at[i],
            halo_rs.at[i],
            (lax.rem(e + 1, groups), t),
            gives,
        )

    def from_first(k):
        sides = ((z, None),) if k == 0 else ((z - k, z >= k), (z + k, z + k < chips))
        for zz, when in sides:
            safe = jnp.clip(zz, 0, chips - 1)
            block = x_buf.at[e1, safe, c]
            wait = functools.partial(received, block, x1_ss.at[safe], x1_rs.at[safe])
            wait() if when is None else pl.when(when)(wait)
            slot = chips + safe
            send(block, block, x2_ss.at[slot], x2_rs.at[slot], (e2, t), when)
            send(block, block, pa_ss.at[slot], pa_rs.at[slot], (e, other), when)

    for k in range(1, chips):
        below, has_below = jnp.maximum(z - k, 0), z >= k
        above, has_above = jnp.minimum(z + k, chips - 1), z + k < chips

        @pl.when(has_below)
        def _():
            received(x_buf.at[e, below, c], up_ss.at[below], up_rs.at[below])

        spread_block(below, True, False, has_below)

        @pl.when(has_above)
        def _():
            received(x_buf.at[e, above, c], dn_ss.at[above], dn_rs.at[above])

        spread_block(above, False, True, has_above)
        from_first(k - 1)
    from_first(chips - 1)

    def spread_weight(zz, up, down, when):
        block = w_buf.at[zz * 2 + c]
        if up:
            ok = z < chips - 1
            ok = ok if when is None else ok & when
            send(block, block, wu_ss.at[zz], wu_rs.at[zz], (e, t + 2), ok)
        if down:
            ok = z > 0
            ok = ok if when is None else ok & when
            send(block, block, wd_ss.at[zz], wd_rs.at[zz], (e, t - 2), ok)
        send(block, block, wp_ss.at[zz], wp_rs.at[zz], (e, other), when)

    def pass_weight(k):
        below, has_below = jnp.maximum(z - k, 0), z >= k
        above, has_above = jnp.minimum(z + k, chips - 1), z + k < chips

        @pl.when(has_below)
        def _():
            received(w_buf.at[below * 2 + c], wu_ss.at[below], wu_rs.at[below])

        spread_weight(below, True, False, has_below)

        @pl.when(has_above)
        def _():
            received(w_buf.at[above * 2 + c], wd_ss.at[above], wd_rs.at[above])

        spread_weight(above, False, True, has_above)

    loads[0].wait()
    spread_weight(z, True, True, None)

    @pl.loop(1, total)
    def _(j):
        source = lax.rem(me + total - j, total)
        received(tiles.at[source], tile_ss.at[j], tile_rs.at[j])

    @pl.loop(1, ranks)
    def _(j):
        source = lax.rem(t + ranks - j, ranks)
        received(qb_buf.at[source], q_ss.at[j], q_rs.at[j])

    lanes = lax.broadcasted_iota(jnp.int32, (WINDOW, 128), 1)
    low = lanes < HEAD_DIM

    def doubled(part, rows, out):
        wide = rows.astype(jnp.float32)
        turned = pltpu.roll(wide, HEAD_DIM, 1)
        place = pl.ds(part * WINDOW, WINDOW)
        out[0, place, :] = jnp.where(low, wide, turned).astype(jnp.bfloat16)
        out[1, place, :] = jnp.where(low, turned, wide).astype(jnp.bfloat16)

    for i, (source, out) in enumerate(((key_ref, kdup), (value_ref, vdup))):
        doubled(1, source[pl.ds(pl.multiple_of(t * WINDOW, WINDOW), WINDOW), :], out)

        @pl.when(t > 0)
        def _():
            before = jnp.maximum(t - 1, 0) * WINDOW
            doubled(0, source[pl.ds(pl.multiple_of(before, WINDOW), WINDOW), :], out)

        @pl.when(takes)
        def _():
            received(halo.at[i], halo_ss.at[i], halo_rs.at[i])
            doubled(0, halo[i], out)

        @pl.when(me == 0)
        def _():
            doubled(0, jnp.zeros((WINDOW, 128), jnp.bfloat16), out)

    query_pos = lax.broadcasted_iota(jnp.int32, (WINDOW, 2 * WINDOW), 0) + WINDOW
    key_pos = lax.broadcasted_iota(jnp.int32, (WINDOW, 2 * WINDOW), 1)
    first = jnp.where(me == 0, WINDOW, 0)
    allowed = (key_pos <= query_pos) & (key_pos > query_pos - WINDOW) & (key_pos >= first)

    @pl.loop(0, ranks)
    def _(j):
        pair = qb_buf[j]
        kept = lax.div(j * KV_HEADS, ranks)
        keys, vals = kdup[kept], vdup[kept]
        outs = []
        for i in range(2):
            mine = low if i == 0 else jnp.logical_not(low)
            query = jnp.where(mine, pair, jnp.zeros_like(pair))
            scores = lax.dot_general(
                query, keys, (((1,), (1,)), ((), ())), preferred_element_type=jnp.float32
            ) * HEAD_DIM ** (-0.5)
            masked = jnp.where(allowed, scores, big_negative)
            sink = tiles[e * ranks + j, groups : groups + 1, i : i + 1]
            row_max = jnp.maximum(jnp.max(masked, -1, keepdims=True), sink)
            powers = jnp.exp(masked - row_max)
            totals = jnp.sum(powers, -1, keepdims=True) + jnp.exp(sink - row_max)
            probs = (powers / totals).astype(jnp.bfloat16)
            outs.append(jnp.dot(probs, vals, preferred_element_type=jnp.float32))
        att[:, pl.ds(pl.multiple_of(j * 128, 128), 128)] = jnp.where(low, outs[0], outs[1]).astype(
            jnp.bfloat16
        )

    for load in loads[1:]:
        load.wait()

    row_count = rows_ref.shape[0]
    width = rows_ref.shape[1]
    diagonal = lax.broadcasted_iota(jnp.int32, (row_count, 128), 0) == lax.broadcasted_iota(
        jnp.int32, (row_count, 128), 1
    )

    def column_of(i):
        xi = x + lax.rem(i, 2) * (1 - 2 * x)
        yi = y + lax.div(i, 2) * (1 - 2 * y)
        return yi * 2 + xi

    def partner_column(slot_column, slot):
        for zz in range(chips):
            where = slot * chips + zz
            received(x_buf.at[slot_column, zz, oc], pa_ss.at[where], pa_rs.at[where])

    def from_second(slot):
        column = e2 if slot == 0 else e3
        for zz in range(chips):
            where = slot * chips + zz
            block = x_buf.at[column, zz, c]
            received(block, x2_ss.at[where], x2_rs.at[where])
            to = (2 + slot) * chips + zz
            remote(block, block, pa_ss.at[to], pa_rs.at[to], (e, other)).start()

    def fold(i):
        column = column_of(i)
        received(r1_buf.at[i], s1_ss.at[i], s1_rs.at[i])
        for zz in range(chips):
            p_buf[column, zz, c] = (
                p_buf[column, zz, c].astype(jnp.float32) + r1_buf[i, zz].astype(jnp.float32)
            ).astype(jnp.bfloat16)

        @pl.when((column == e2) | (column == e3))
        def _():
            slot = jnp.where(column == e3, 1, 0)
            remote(
                p_buf.at[column, :, c], r2_buf.at[slot], s2_ss.at[slot], s2_rs.at[slot], (e2, t)
            ).start()

    @pl.loop(0, groups)
    def _(i):
        column = column_of(i)

        @pl.when(i == 0)
        def _():
            partner_column(e, 0)

        @pl.when(i == 1)
        def _():
            from_second(0)
            partner_column(e1, 2)
            partner_column(e2, 1)

        @pl.when(i == 3)
        def _():
            from_second(1)
            partner_column(e3, 3)

        rows = x_buf[column].reshape(ranks * row_count, width)
        gate_val = jnp.dot(rows, gate_w[...], preferred_element_type=jnp.float32)
        up_val = jnp.dot(rows, up_w[...], preferred_element_type=jnp.float32)
        hidden = (gate_val / (1.0 + jnp.exp(-gate_val)) * up_val).astype(jnp.bfloat16)
        shares = []
        for j in range(ranks):
            line = tiles[column * ranks + j, pl.ds(e, 1), :]
            shares.append(
                jnp.sum(
                    jnp.where(diagonal, jnp.broadcast_to(line, (row_count, 128)), 0.0),
                    -1,
                    keepdims=True,
                )
            )
        share = jnp.concatenate(shares, 0)
        down = jnp.dot(hidden, down_w[...], preferred_element_type=jnp.float32)
        p_buf[column] = (
            (down * share).astype(jnp.bfloat16).reshape(chips, 2, row_count, width)
        )
        remote(
            p_buf.at[column, :, oc], r1_buf.at[i], s1_ss.at[i], s1_rs.at[i], (e, other)
        ).start()

        @pl.when(i > 0)
        def _():
            fold(i - 1)

    if chips > 1:
        pass_weight(1)
    fold(groups - 1)

    def add_in(block, extra):
        block[...] = (block[...].astype(jnp.float32) + extra[...].astype(jnp.float32)).astype(
            jnp.bfloat16
        )

    received(r2_buf.at[1], s2_ss.at[1], s2_rs.at[1])
    for zz in range(chips):
        add_in(p_buf.at[e1, zz, c], r2_buf.at[1, zz])
    send(p_buf.at[e1, :, c], r3_buf, s3_ss.at[0], s3_rs.at[0], (e1, t))
    received(r2_buf.at[0], s2_ss.at[0], s2_rs.at[0])
    for zz in range(chips):
        add_in(p_buf.at[e, zz, c], r2_buf.at[0, zz])
    if chips > 2:
        pass_weight(2)
    received(r3_buf, s3_ss.at[0], s3_rs.at[0])
    for zz in range(chips):
        add_in(p_buf.at[e, zz, c], r3_buf.at[zz])

    for k in range(chips - 1):
        for zz, mine, inner, buf, ss, rs, to in (
            (chips - 1 - k, z < chips - 1 - k, z > 0, ru_buf, ru_ss, ru_rs, t + 2),
            (k, z > k, z < chips - 1, rd_buf, rd_ss, rd_rs, t - 2),
        ):

            @pl.when(mine & inner)
            def _():
                received(buf.at[zz], ss.at[zz], rs.at[zz])
                add_in(p_buf.at[e, zz, c], buf.at[zz])

            send(p_buf.at[e, zz, c], buf.at[zz], ss.at[zz], rs.at[zz], (e, to), mine)

    for k in range(3, chips):
        pass_weight(k)
    for zz in range(chips):
        received(w_buf.at[zz * 2 + oc], wp_ss.at[zz], wp_rs.at[zz])
    mix_ref[...] = jnp.dot(
        att[...], w_buf[...].reshape(ranks * 128, width), preferred_element_type=jnp.float32
    ).astype(jnp.bfloat16)

    @pl.when(z > 0)
    def _():
        received(ru_buf.at[z], ru_ss.at[z], ru_rs.at[z])
        add_in(p_buf.at[e, z, c], ru_buf.at[z])

    @pl.when(z < chips - 1)
    def _():
        received(rd_buf.at[z], rd_ss.at[z], rd_rs.at[z])
        add_in(p_buf.at[e, z, c], rd_buf.at[z])

    moe_ref[...] = p_buf[e, z, c]

    for when, copy in pending:
        copy.wait_send() if when is None else pl.when(when)(copy.wait_send)
    for slot in range(2 * chips, 4 * chips):
        block = x_buf.at[e, z, c]
        remote(block, block, pa_ss.at[slot], pa_rs.at[slot], (e, other)).wait_send()

    @pl.loop(0, groups)
    def _(i):
        remote(
            p_buf.at[e, :, oc], r1_buf.at[i], s1_ss.at[i], s1_rs.at[i], (e, other)
        ).wait_send()

    for slot in range(2):
        remote(
            p_buf.at[e2, :, c], r2_buf.at[slot], s2_ss.at[slot], s2_rs.at[slot], (e2, t)
        ).wait_send()

    @pl.loop(1, ranks)
    def _(j):
        remote(qb_buf.at[t], qb_buf.at[t], q_ss.at[j], q_rs.at[j], (e, other)).wait_send()

    @pl.loop(1, total)
    def _(j):
        remote(tile_ref, tiles.at[me], tile_ss.at[j], tile_rs.at[j], (e, other)).wait_send()


def fused(
    queries,
    key_rows,
    value_rows,
    sink_logits,
    out_weight,
    moe_rows,
    moe_gain,
    routes,
    route_weight,
    gate_weight,
    up_weight,
    down_weight,
):
    groups, ranks = lax.axis_size("ep"), lax.axis_size("tp")
    chips, total = ranks // 2, groups * ranks
    row_count, width = moe_rows.shape
    units = gate_weight.shape[2]
    chosen, weights = routes.T, route_weight.T
    named = chosen[:, None, :] == jnp.arange(groups, dtype=jnp.int32)[None, :, None]
    shares = jnp.sum(jnp.where(named, weights[:, None, :], 0.0), 0)
    tile_rows = -(-(groups + 1) // 8) * 8
    shares = jnp.pad(shares, ((0, tile_rows - groups), (0, 128 - row_count)))
    sinks = jnp.pad(
        sink_logits[None, :], ((groups, tile_rows - groups - 1), (0, 128 - sink_logits.shape[0]))
    )
    tile = shares + sinks
    bf16, f32 = jnp.bfloat16, jnp.float32
    vmem = pltpu.VMEM
    dma = pltpu.SemaphoreType.DMA
    sems = [(4,)]
    for count in (
        total,
        ranks,
        2,
        chips,
        chips,
        4 * chips,
        chips,
        2 * chips,
        chips,
        chips,
        chips,
        groups,
        2,
        1,
        chips,
        chips,
    ):
        sems += [(count,), (count,)]
    block = (row_count, width)
    in_vmem = pl.BlockSpec(memory_space=pltpu.VMEM)
    in_any = pl.BlockSpec(memory_space=pl.ANY)
    return pl.pallas_call(
        functools.partial(fused_kernel, groups, ranks),
        out_shape=(
            jax.ShapeDtypeStruct((queries.shape[0] // ranks, width), bf16),
            jax.ShapeDtypeStruct(block, bf16),
        ),
        in_specs=[in_vmem] * 6 + [in_any] * 4,
        out_specs=(in_vmem, in_vmem),
        scratch_shapes=[
            vmem((groups, chips, 2) + block, bf16),
            vmem((groups, chips, 2) + block, bf16),
            vmem((groups, chips) + block, bf16),
            vmem((2, chips) + block, bf16),
            vmem((chips,) + block, bf16),
            vmem((chips,) + block, bf16),
            vmem((chips,) + block, bf16),
            vmem((ranks,) + out_weight.shape, bf16),
            vmem((ranks, WINDOW, 128), bf16),
            vmem((total, tile_rows, 128), f32),
            vmem((2, WINDOW, 128), bf16),
            vmem((2, 2 * WINDOW, 128), bf16),
            vmem((2, 2 * WINDOW, 128), bf16),
            vmem((WINDOW, ranks * 128), bf16),
            vmem((width, units), bf16),
            vmem((width, units), bf16),
            vmem((units, width), bf16),
        ]
        + [dma(shape) for shape in sems],
        compiler_params=pltpu.CompilerParams(
            collective_id=0, has_side_effects=True, vmem_limit_bytes=60 * 1024 * 1024
        ),
    )(
        queries,
        key_rows,
        value_rows,
        tile,
        moe_rows,
        moe_gain[None, :],
        out_weight,
        gate_weight,
        up_weight,
        down_weight,
    )


def body(
    queries,
    key_rows,
    value_rows,
    sink_logits,
    out_weight,
    moe_rows,
    moe_gain,
    routes,
    route_weight,
    gate_weight,
    up_weight,
    down_weight,
):
    groups, ranks = lax.axis_size("ep"), lax.axis_size("tp")
    fits = groups == 4 and ranks % 2 == 0 and ranks <= 8
    fits = fits and queries.shape == (ranks * WINDOW, 2 * HEAD_DIM)
    fits = fits and key_rows.shape[1] == 128 and moe_rows.shape[0] % 16 == 0
    if fits:
        return fused(
            queries,
            key_rows,
            value_rows,
            sink_logits,
            out_weight,
            moe_rows,
            moe_gain,
            routes,
            route_weight,
            gate_weight,
            up_weight,
            down_weight,
        )
    mixer_out = mixer(queries, key_rows, value_rows, sink_logits, out_weight)
    moe_out = experts(moe_rows, moe_gain, routes, route_weight, gate_weight, up_weight, down_weight)
    return (mixer_out, moe_out)


def solution(mesh):
    in_specs = (
        P("ep", "tp"),
        P("ep", None),
        P("ep", None),
        P("tp"),
        P("tp", None),
        P(("ep", "tp"), None),
        P(),
        P(("ep", "tp"), None),
        P(("ep", "tp"), None),
        P("ep", None, "tp"),
        P("ep", None, "tp"),
        P("ep", "tp", None),
    )
    out_specs = (P(("ep", "tp"), None), P(("ep", "tp"), None))
    return jax.shard_map(body, mesh=mesh, in_specs=in_specs, out_specs=out_specs, check_vma=False)
```

```python
import functools

import jax
import jax.numpy as jnp
from jax import lax
from jax.experimental import pallas as pl
from jax.experimental.pallas import tpu as pltpu
from jax.sharding import PartitionSpec as P

MESH = pl.DeviceIdType.MESH

HEADS = 16
KV_HEADS = 2
HEAD_DIM = 64
WINDOW = 128
TOP = 2


big_negative = -1e30
norm_eps = 1e-05


def passed_along(value, axis, steps):
    count = lax.axis_size(axis)
    initial, last = (max(0, -steps), min(count, count - steps))
    return lax.ppermute(value, axis, [(source, source + steps) for source in range(initial, last)])


def layer_normed(inputs, gain):
    values = inputs.astype(jnp.float32)
    center = values - jnp.mean(values, -1, keepdims=True)
    spread = jnp.mean(center * center, -1, keepdims=True)
    return (center * lax.rsqrt(spread + norm_eps) * gain).astype(jnp.bfloat16)


def attend(queries, key_rows, value_rows, sink_logits):
    total = queries.shape[0]
    heads_here = sink_logits.shape[0]
    blocks = total // WINDOW
    key_head = lax.axis_index("tp") * heads_here // (HEADS // KV_HEADS)
    key_own = lax.dynamic_slice_in_dim(key_rows, key_head * HEAD_DIM, HEAD_DIM, 1)
    value_own = lax.dynamic_slice_in_dim(value_rows, key_head * HEAD_DIM, HEAD_DIM, 1)
    last_rows = jnp.concatenate([key_own[total - WINDOW :], value_own[total - WINDOW :]], 1)
    earlier = passed_along(last_rows, "ep", 1)
    key_ext = jnp.concatenate([earlier[:, :HEAD_DIM], key_own], 0)
    value_ext = jnp.concatenate([earlier[:, HEAD_DIM:], value_own], 0)
    key_blocks = jnp.concatenate(
        [
            key_ext[:total].reshape(blocks, WINDOW, HEAD_DIM),
            key_ext[WINDOW:].reshape(blocks, WINDOW, HEAD_DIM),
        ],
        1,
    )
    value_blocks = jnp.concatenate(
        [
            value_ext[:total].reshape(blocks, WINDOW, HEAD_DIM),
            value_ext[WINDOW:].reshape(blocks, WINDOW, HEAD_DIM),
        ],
        1,
    )
    query_blocks = queries.reshape(blocks, WINDOW, heads_here, HEAD_DIM)
    scores = jnp.einsum(
        "nqhd,nkd->nhqk", query_blocks, key_blocks, preferred_element_type=jnp.float32
    ) * HEAD_DIM ** (-0.5)
    anchor = lax.axis_index("ep") * total
    block_base = anchor + jnp.arange(blocks, dtype=jnp.int32)[:, None, None] * WINDOW
    query_pos = block_base + jnp.arange(WINDOW, dtype=jnp.int32)[None, :, None]
    key_pos = block_base - WINDOW + jnp.arange(2 * WINDOW, dtype=jnp.int32)[None, None, :]
    allowed = ((key_pos <= query_pos) & (key_pos > query_pos - WINDOW) & (key_pos >= 0))[:, None]
    masked = jnp.where(allowed, scores, big_negative)
    sinks = sink_logits[None, :, None]
    row_max = jnp.maximum(jnp.max(masked, -1), sinks)
    powers = jnp.where(allowed, jnp.exp(masked - row_max[..., None]), 0.0)
    totals = jnp.sum(powers, -1) + jnp.exp(sinks - row_max)
    attn_probs = (powers / totals[..., None]).astype(jnp.bfloat16)
    attended = jnp.einsum(
        "nhqk,nkd->nqhd", attn_probs, value_blocks, preferred_element_type=jnp.float32
    )
    return attended.astype(jnp.bfloat16).reshape(total, heads_here * HEAD_DIM)


def mixer(queries, key_rows, value_rows, sink_logits, out_weight):
    attended = attend(queries, key_rows, value_rows, sink_logits)
    return lax.psum_scatter(
        jnp.dot(attended, out_weight, preferred_element_type=jnp.float32).astype(jnp.bfloat16),
        "tp",
        scatter_dimension=0,
        tiled=True,
    )


def experts(moe_rows, moe_gain, routes, route_weight, gate_weight, up_weight, down_weight):
    row_count = moe_rows.shape[0]
    width_all = moe_rows.shape[1]
    expert_count = gate_weight.shape[0] * lax.axis_size("ep")
    capacity = 3 * row_count * TOP // (2 * expert_count)
    normed = layer_normed(moe_rows, moe_gain)
    chosen = routes.reshape(-1)
    onehot = (chosen[:, None] == jnp.arange(expert_count, dtype=jnp.int32)[None, :]).astype(
        jnp.int32
    )
    earlier_count = jnp.cumsum(onehot, 0) - onehot
    slot_index = jnp.sum(earlier_count * onehot, 1)
    target = chosen * capacity + slot_index
    matches = target[None, :] == jnp.arange(expert_count * capacity, dtype=jnp.int32)[:, None]
    dispatch_map = jnp.sum(matches.reshape(expert_count * capacity, row_count, TOP), -1).astype(
        jnp.bfloat16
    )
    buffer = jnp.dot(dispatch_map, normed, preferred_element_type=jnp.float32).astype(jnp.bfloat16)
    buffer = buffer.reshape(expert_count, capacity, width_all)
    gate_mat = gate_weight[0]
    up_mat = up_weight[0]
    down_mat = down_weight[0]
    received = lax.all_to_all(buffer, "ep", split_axis=0, concat_axis=0, tiled=True)
    total = received.shape[0] * received.shape[1]
    flat_rows = received.reshape(total, width_all)
    shard_rows = lax.all_gather(flat_rows, "tp", axis=0, tiled=True)
    gate_val = jnp.dot(shard_rows, gate_mat, preferred_element_type=jnp.float32)
    up_val = jnp.dot(shard_rows, up_mat, preferred_element_type=jnp.float32)
    hidden = (jax.nn.silu(gate_val) * up_val).astype(jnp.bfloat16)
    summed = lax.psum_scatter(
        jnp.dot(hidden, down_mat, preferred_element_type=jnp.float32).astype(jnp.bfloat16),
        "tp",
        scatter_dimension=0,
        tiled=True,
    )
    results = summed.reshape(received.shape)
    returned = lax.all_to_all(results, "ep", split_axis=0, concat_axis=0, tiled=True)
    weights_flat = route_weight.reshape(-1)
    combine_map = jnp.sum(
        jnp.where(matches, weights_flat[None, :], 0.0).reshape(
            expert_count * capacity, row_count, TOP
        ),
        -1,
    )
    returned_flat = returned.reshape(expert_count * capacity, width_all).astype(jnp.float32)
    moe_out = lax.dot_general(
        combine_map, returned_flat, (((0,), (0,)), ((), ())), precision=lax.Precision.HIGHEST
    )
    return moe_out.astype(jnp.bfloat16)


def fused_kernel(
    groups,
    ranks,
    q_ref,
    key_ref,
    value_ref,
    tile_ref,
    rows_ref,
    gain_ref,
    ow_hbm,
    gate_hbm,
    up_hbm,
    down_hbm,
    mix_ref,
    moe_ref,
    x_buf,
    p_buf,
    r1_buf,
    r2_buf,
    r3_buf,
    ru_buf,
    rd_buf,
    w_buf,
    qb_buf,
    tiles,
    halo,
    kdup,
    vdup,
    att,
    gate_w,
    up_w,
    down_w,
    load_sem,
    tile_ss,
    tile_rs,
    q_ss,
    q_rs,
    halo_ss,
    halo_rs,
    up_ss,
    up_rs,
    dn_ss,
    dn_rs,
    pa_ss,
    pa_rs,
    x1_ss,
    x1_rs,
    x2_ss,
    x2_rs,
    wu_ss,
    wu_rs,
    wd_ss,
    wd_rs,
    wp_ss,
    wp_rs,
    wx_ss,
    wx_rs,
    wq_ss,
    wq_rs,
    s1_ss,
    s1_rs,
    s2_ss,
    s2_rs,
    s3_ss,
    s3_rs,
    ru_ss,
    ru_rs,
    rd_ss,
    rd_rs,
):
    chips = ranks // 2
    total = groups * ranks
    e, t = lax.axis_index("ep"), lax.axis_index("tp")
    z, c = lax.div(t, 2), lax.rem(t, 2)
    y, x = lax.div(e, 2), lax.rem(e, 2)
    me = e * ranks + t
    ex, ey, e3 = e + 1 - 2 * x, e + 2 - 4 * y, 3 - e
    e1 = ex * (1 - c) + ey * c
    e2 = ey * (1 - c) + ex * c
    other = t + 1 - 2 * c
    oc = 1 - c
    columns = (e, e1, e2, e3)
    pending = []

    def remote(src, dst, ss, rs, to):
        return pltpu.make_async_remote_copy(
            src_ref=src, dst_ref=dst, send_sem=ss, recv_sem=rs, device_id=to, device_id_type=MESH
        )

    def send(src, dst, ss, rs, to, when=None):
        copy = remote(src, dst, ss, rs, to)
        pending.append((when, copy))
        if when is None:
            copy.start()
        else:
            pl.when(when)(copy.start)

    def received(dst, ss, rs):
        remote(dst, dst, ss, rs, (e, other)).wait_recv()

    loads = [
        pltpu.make_async_copy(ow_hbm, w_buf.at[t], load_sem.at[0]),
        pltpu.make_async_copy(gate_hbm.at[0], gate_w, load_sem.at[1]),
        pltpu.make_async_copy(up_hbm.at[0], up_w, load_sem.at[2]),
        pltpu.make_async_copy(down_hbm.at[0], down_w, load_sem.at[3]),
    ]
    for load in loads:
        load.start()

    barrier = pltpu.get_barrier_semaphore()

    @pl.loop(1, total)
    def _(j):
        to = lax.rem(me + j, total)
        pl.semaphore_signal(
            barrier,
            inc=1,
            device_id=(lax.div(to, ranks), lax.rem(to, ranks)),
            device_id_type=MESH,
        )

    values = rows_ref[...].astype(jnp.float32)
    center = values - jnp.mean(values, -1, keepdims=True)
    spread = jnp.mean(center * center, -1, keepdims=True)
    x_buf[e, z, c] = (center * lax.rsqrt(spread + norm_eps) * gain_ref[...]).astype(jnp.bfloat16)
    tiles[me] = tile_ref[...]
    qb_buf[t] = q_ref[pl.ds(pl.multiple_of(t * WINDOW, WINDOW), WINDOW), :]

    pl.semaphore_wait(barrier, total - 1)

    piece_rows = rows_ref.shape[0] // 2

    def spread_block(zz, up, down, when):
        block = x_buf.at[e, zz, c]
        if up:
            ok = z < chips - 1
            ok = ok if when is None else ok & when
            for h in range(2):
                part = block.at[pl.ds(h * piece_rows, piece_rows), :]
                at = zz * 2 + h
                if when is not None:
                    wait = functools.partial(received, part, up_ss.at[at], up_rs.at[at])
                    pl.when(when)(wait)
                send(part, part, up_ss.at[at], up_rs.at[at], (e, t + 2), ok)
        if down:
            ok = z > 0
            ok = ok if when is None else ok & when
            for h in range(2):
                part = block.at[pl.ds(h * piece_rows, piece_rows), :]
                at = zz * 2 + h
                if when is not None:
                    wait = functools.partial(received, part, dn_ss.at[at], dn_rs.at[at])
                    pl.when(when)(wait)
                send(part, part, dn_ss.at[at], dn_rs.at[at], (e, t - 2), ok)
        send(block, block, x1_ss.at[zz], x1_rs.at[zz], (e1, t), when)
        send(block, block, x2_ss.at[zz], x2_rs.at[zz], (e2, t), when)
        send(block, block, pa_ss.at[zz], pa_rs.at[zz], (e, other), when)

    spread_block(z, True, True, None)

    last = key_ref.shape[0] - WINDOW
    gives = (t == 0) & (e < groups - 1)
    takes = (t == 0) & (e > 0)
    for i, source in enumerate((key_ref, value_ref)):
        send(
            source.at[pl.ds(last, WINDOW), :],
            halo.at[i],
            halo_ss.at[i],
            halo_rs.at[i],
            (lax.rem(e + 1, groups), t),
            gives,
        )

    def from_first(k):
        sides = ((z, None),) if k == 0 else ((z - k, z >= k), (z + k, z + k < chips))
        for zz, when in sides:
            safe = jnp.clip(zz, 0, chips - 1)
            block = x_buf.at[e1, safe, c]
            wait = functools.partial(received, block, x1_ss.at[safe], x1_rs.at[safe])
            wait() if when is None else pl.when(when)(wait)
            slot = chips + safe
            send(block, block, x2_ss.at[slot], x2_rs.at[slot], (e2, t), when)
            send(block, block, pa_ss.at[slot], pa_rs.at[slot], (e, other), when)

    third = w_buf.shape[1] // 4
    side = x * (1 - c) + y * c
    carried = pl.ds(pl.multiple_of(side * third, third), 3 * third)
    given = pl.ds(pl.multiple_of(3 * side * third, third), third)
    taken = pl.ds(pl.multiple_of(3 * (1 - side) * third, third), third)

    other_side = x * c + y * (1 - c)
    other_carried = pl.ds(pl.multiple_of(other_side * third, third), 3 * third)
    other_taken = pl.ds(pl.multiple_of(3 * (1 - other_side) * third, third), third)

    def weight_copies(zz, up, down, when):
        block = w_buf.at[zz * 2 + c, carried, :]
        copies = []
        if up:
            ok = z < chips - 1
            ok = ok if when is None else ok & when
            copies.append((ok, remote(block, block, wu_ss.at[zz], wu_rs.at[zz], (e, t + 2))))
        if down:
            ok = z > 0
            ok = ok if when is None else ok & when
            copies.append((ok, remote(block, block, wd_ss.at[zz], wd_rs.at[zz], (e, t - 2))))
        copies.append((when, remote(block, block, wp_ss.at[zz], wp_rs.at[zz], (e, other))))
        if when is None:
            rest = w_buf.at[zz * 2 + c, taken, :]
            copies.append((when, remote(rest, rest, wq_ss.at[zz], wq_rs.at[zz], (e, other))))
        else:
            piece = w_buf.at[zz * 2 + c, given, :]
            copies.append((when, remote(piece, piece, wx_ss.at[zz], wx_rs.at[zz], (e1, t))))
        return copies

    def spread_weight(zz, up, down, when):
        for ok, copy in weight_copies(zz, up, down, when):
            copy.start() if ok is None else pl.when(ok)(copy.start)

    def pass_weight(k):
        below, has_below = jnp.maximum(z - k, 0), z >= k
        above, has_above = jnp.minimum(z + k, chips - 1), z + k < chips

        @pl.when(has_below)
        def _():
            received(w_buf.at[below * 2 + c, carried, :], wu_ss.at[below], wu_rs.at[below])

        spread_weight(below, True, False, has_below)

        @pl.when(has_above)
        def _():
            received(w_buf.at[above * 2 + c, carried, :], wd_ss.at[above], wd_rs.at[above])

        spread_weight(above, False, True, has_above)

    for k in range(1, chips):
        below, has_below = jnp.maximum(z - k, 0), z >= k
        above, has_above = jnp.minimum(z + k, chips - 1), z + k < chips

        spread_block(below, True, False, has_below)

        spread_block(above, False, True, has_above)
        from_first(k - 1)
    from_first(chips - 1)

    @pl.loop(1, total)
    def _(j):
        to = lax.rem(me + j, total)
        remote(
            tile_ref,
            tiles.at[me],
            tile_ss.at[j],
            tile_rs.at[j],
            (lax.div(to, ranks), lax.rem(to, ranks)),
        ).start()

    @pl.loop(1, ranks)
    def _(j):
        tt = lax.rem(t + j, ranks)
        remote(
            q_ref.at[pl.ds(pl.multiple_of(tt * WINDOW, WINDOW), WINDOW), :],
            qb_buf.at[t],
            q_ss.at[j],
            q_rs.at[j],
            (e, tt),
        ).start()

    loads[0].wait()
    spread_weight(z, True, True, None)


    for load in loads[1:]:
        load.wait()

    row_count = rows_ref.shape[0]
    width = rows_ref.shape[1]
    diagonal = lax.broadcasted_iota(jnp.int32, (row_count, 128), 0) == lax.broadcasted_iota(
        jnp.int32, (row_count, 128), 1
    )

    def column_of(i):
        xi = x + lax.rem(i, 2) * (1 - 2 * x)
        yi = y + lax.div(i, 2) * (1 - 2 * y)
        return yi * 2 + xi

    def partner_column(slot_column, slot):
        for zz in range(chips):
            where = slot * chips + zz
            received(x_buf.at[slot_column, zz, oc], pa_ss.at[where], pa_rs.at[where])

    def from_second(slot):
        column = e2 if slot == 0 else e3
        for zz in range(chips):
            where = slot * chips + zz
            block = x_buf.at[column, zz, c]
            received(block, x2_ss.at[where], x2_rs.at[where])
            to = (2 + slot) * chips + zz
            remote(block, block, pa_ss.at[to], pa_rs.at[to], (e, other)).start()

    far_first = []
    for k in range(chips - 1, 0, -1):
        far_first.append((jnp.maximum(z - k, 0), z >= k))
        far_first.append((jnp.minimum(z + k, chips - 1), z + k < chips))
    far_first.append((z, None))

    def fold(i):
        column = column_of(i)
        received(r1_buf.at[i], s1_ss.at[i], s1_rs.at[i])
        for zz in range(chips):
            p_buf[column, zz, c] = (
                p_buf[column, zz, c].astype(jnp.float32) + r1_buf[i, zz].astype(jnp.float32)
            ).astype(jnp.bfloat16)

        @pl.when((column == e2) | (column == e3))
        def _():
            slot = jnp.where(column == e3, 1, 0)
            for zz, when in far_first:
                place = slot * chips + zz
                copy = remote(
                    p_buf.at[column, zz, c],
                    r2_buf.at[slot, zz],
                    s2_ss.at[place],
                    s2_rs.at[place],
                    (e2, t),
                )
                copy.start() if when is None else pl.when(when)(copy.start)

    @pl.loop(0, groups)
    def _(i):
        column = column_of(i)

        @pl.when(i == 0)
        def _():
            partner_column(e, 0)

        @pl.when(i == 1)
        def _():
            from_second(0)
            partner_column(e1, 2)
            partner_column(e2, 1)

        @pl.when(i == 3)
        def _():
            from_second(1)
            partner_column(e3, 3)

        if chips > 1:

            @pl.when(i == 2)
            def _():
                pass_weight(1)

        rows = x_buf[column].reshape(ranks * row_count, width)
        gate_val = jnp.dot(rows, gate_w[...], preferred_element_type=jnp.float32)
        up_val = jnp.dot(rows, up_w[...], preferred_element_type=jnp.float32)
        hidden = (gate_val / (1.0 + jnp.exp(-gate_val)) * up_val).astype(jnp.bfloat16)

        @pl.when(i > 0)
        def _():
            fold(i - 1)

        @pl.when(i == 0)
        def _():
            @pl.loop(1, total)
            def _(j):
                source = lax.rem(me + total - j, total)
                received(tiles.at[source], tile_ss.at[j], tile_rs.at[j])

        shares = []
        for j in range(ranks):
            line = tiles[column * ranks + j, pl.ds(e, 1), :]
            shares.append(
                jnp.sum(
                    jnp.where(diagonal, jnp.broadcast_to(line, (row_count, 128)), 0.0),
                    -1,
                    keepdims=True,
                )
            )
        share = jnp.concatenate(shares, 0)
        down = jnp.dot(hidden, down_w[...], preferred_element_type=jnp.float32)
        p_buf[column] = (
            (down * share).astype(jnp.bfloat16).reshape(chips, 2, row_count, width)
        )
        remote(
            p_buf.at[column, :, oc], r1_buf.at[i], s1_ss.at[i], s1_rs.at[i], (e, other)
        ).start()

    fold(groups - 1)
    if chips > 2:
        pass_weight(2)

    @pl.loop(1, ranks)
    def _(j):
        source = lax.rem(t + ranks - j, ranks)
        received(qb_buf.at[source], q_ss.at[j], q_rs.at[j])

    lanes = lax.broadcasted_iota(jnp.int32, (WINDOW, 128), 1)
    low = lanes < HEAD_DIM

    def doubled(part, rows, out):
        wide = rows.astype(jnp.float32)
        turned = pltpu.roll(wide, HEAD_DIM, 1)
        place = pl.ds(part * WINDOW, WINDOW)
        out[0, place, :] = jnp.where(low, wide, turned).astype(jnp.bfloat16)
        out[1, place, :] = jnp.where(low, turned, wide).astype(jnp.bfloat16)

    for i, (source, out) in enumerate(((key_ref, kdup), (value_ref, vdup))):
        doubled(1, source[pl.ds(pl.multiple_of(t * WINDOW, WINDOW), WINDOW), :], out)

        @pl.when(t > 0)
        def _():
            before = jnp.maximum(t - 1, 0) * WINDOW
            doubled(0, source[pl.ds(pl.multiple_of(before, WINDOW), WINDOW), :], out)

        @pl.when(takes)
        def _():
            received(halo.at[i], halo_ss.at[i], halo_rs.at[i])
            doubled(0, halo[i], out)

        @pl.when(me == 0)
        def _():
            doubled(0, jnp.zeros((WINDOW, 128), jnp.bfloat16), out)

    query_pos = lax.broadcasted_iota(jnp.int32, (WINDOW, 2 * WINDOW), 0) + WINDOW
    key_pos = lax.broadcasted_iota(jnp.int32, (WINDOW, 2 * WINDOW), 1)
    first = jnp.where(me == 0, WINDOW, 0)
    allowed = (key_pos <= query_pos) & (key_pos > query_pos - WINDOW) & (key_pos >= first)

    def attend_pairs(begin, end):
        @pl.loop(begin, end)
        def _(j):
            pair = qb_buf[j]
            kept = lax.div(j * KV_HEADS, ranks)
            keys, vals = kdup[kept], vdup[kept]
            outs = []
            for i in range(2):
                mine = low if i == 0 else jnp.logical_not(low)
                query = jnp.where(mine, pair, jnp.zeros_like(pair))
                scores = lax.dot_general(
                    query, keys, (((1,), (1,)), ((), ())), preferred_element_type=jnp.float32
                ) * HEAD_DIM ** (-0.5)
                masked = jnp.where(allowed, scores, big_negative)
                sink = tiles[e * ranks + j, groups : groups + 1, i : i + 1]
                row_max = jnp.maximum(jnp.max(masked, -1, keepdims=True), sink)
                powers = jnp.exp(masked - row_max)
                totals = jnp.sum(powers, -1, keepdims=True) + jnp.exp(sink - row_max)
                probs = (powers / totals).astype(jnp.bfloat16)
                outs.append(jnp.dot(probs, vals, preferred_element_type=jnp.float32))
            att[:, pl.ds(pl.multiple_of(j * 128, 128), 128)] = jnp.where(low, outs[0], outs[1]).astype(
                jnp.bfloat16
            )

    half_pairs = ranks // 2
    attend_pairs(0, half_pairs)

    def add_in(block, extra):
        block[...] = (block[...].astype(jnp.float32) + extra[...].astype(jnp.float32)).astype(
            jnp.bfloat16
        )

    for n, (zz, when) in enumerate(far_first):

        def second(zz=zz):
            received(r2_buf.at[1, zz], s2_ss.at[chips + zz], s2_rs.at[chips + zz])
            add_in(p_buf.at[e1, zz, c], r2_buf.at[1, zz])

        second() if when is None else pl.when(when)(second)
        send(p_buf.at[e1, zz, c], r3_buf.at[zz], s3_ss.at[zz], s3_rs.at[zz], (e1, t), when)
        if n % 2:
            step = (n + 1) // 2
            attend_pairs(
                half_pairs + step * half_pairs // (chips + 1),
                half_pairs + (step + 1) * half_pairs // (chips + 1),
            )

    for n, (zz, when) in enumerate(far_first):

        def third_sum(zz=zz):
            received(r2_buf.at[0, zz], s2_ss.at[zz], s2_rs.at[zz])
            received(r3_buf.at[zz], s3_ss.at[zz], s3_rs.at[zz])
            block = p_buf.at[e, zz, c]
            block[...] = (
                block[...].astype(jnp.float32)
                + r2_buf[0, zz].astype(jnp.float32)
                + r3_buf[zz].astype(jnp.float32)
            ).astype(jnp.bfloat16)

        third_sum() if when is None else pl.when(when)(third_sum)
        if when is None:
            continue
        if n % 2:
            inner, buf, ss, rs, to = z > 0, ru_buf, ru_ss, ru_rs, t + 2
        else:
            inner, buf, ss, rs, to = z < chips - 1, rd_buf, rd_ss, rd_rs, t - 2

        for h in range(2):
            rows = pl.ds(h * piece_rows, piece_rows)
            at = zz * 2 + h

            def chain_sum(zz=zz, rows=rows, at=at):
                received(buf.at[zz, rows, :], ss.at[at], rs.at[at])
                add_in(p_buf.at[e, zz, c, rows, :], buf.at[zz, rows, :])

            pl.when(when & inner)(chain_sum)
            send(
                p_buf.at[e, zz, c, rows, :], buf.at[zz, rows, :], ss.at[at], rs.at[at], (e, to), when
            )

    attend_pairs(half_pairs + chips * half_pairs // (chips + 1), ranks)
    for k in range(3, chips):
        pass_weight(k)
    for zz in range(chips):

        @pl.when(z != zz)
        def _():
            received(w_buf.at[zz * 2 + c, taken, :], wx_ss.at[zz], wx_rs.at[zz])

        rest = w_buf.at[zz * 2 + c, taken, :]
        send(rest, rest, wq_ss.at[zz], wq_rs.at[zz], (e, other), z != zz)
    for zz in range(chips):
        received(w_buf.at[zz * 2 + oc, other_carried, :], wp_ss.at[zz], wp_rs.at[zz])
        received(w_buf.at[zz * 2 + oc, other_taken, :], wq_ss.at[zz], wq_rs.at[zz])
    mix_ref[...] = jnp.dot(
        att[...], w_buf[...].reshape(ranks * 128, width), preferred_element_type=jnp.float32
    ).astype(jnp.bfloat16)

    @pl.when(z > 0)
    def _():
        for h in range(2):
            part = ru_buf.at[z, pl.ds(h * piece_rows, piece_rows), :]
            received(part, ru_ss.at[z * 2 + h], ru_rs.at[z * 2 + h])
        add_in(p_buf.at[e, z, c], ru_buf.at[z])

    @pl.when(z < chips - 1)
    def _():
        for h in range(2):
            part = rd_buf.at[z, pl.ds(h * piece_rows, piece_rows), :]
            received(part, rd_ss.at[z * 2 + h], rd_rs.at[z * 2 + h])
        add_in(p_buf.at[e, z, c], rd_buf.at[z])

    moe_ref[...] = p_buf[e, z, c]

    pending.extend(weight_copies(z, True, True, None))
    for k in range(1, chips):
        pending.extend(weight_copies(jnp.maximum(z - k, 0), True, False, z >= k))
        pending.extend(
            weight_copies(jnp.minimum(z + k, chips - 1), False, True, z + k < chips)
        )
    for when, copy in pending:
        copy.wait_send() if when is None else pl.when(when)(copy.wait_send)
    for slot in range(2 * chips, 4 * chips):
        block = x_buf.at[e, z, c]
        remote(block, block, pa_ss.at[slot], pa_rs.at[slot], (e, other)).wait_send()

    @pl.loop(0, groups)
    def _(i):
        remote(
            p_buf.at[e, :, oc], r1_buf.at[i], s1_ss.at[i], s1_rs.at[i], (e, other)
        ).wait_send()

    for place in range(2 * chips):
        remote(
            p_buf.at[e2, 0, c], r2_buf.at[0, 0], s2_ss.at[place], s2_rs.at[place], (e2, t)
        ).wait_send()

    @pl.loop(1, ranks)
    def _(j):
        remote(qb_buf.at[t], qb_buf.at[t], q_ss.at[j], q_rs.at[j], (e, other)).wait_send()

    @pl.loop(1, total)
    def _(j):
        remote(tile_ref, tiles.at[me], tile_ss.at[j], tile_rs.at[j], (e, other)).wait_send()


def fused(
    queries,
    key_rows,
    value_rows,
    sink_logits,
    out_weight,
    moe_rows,
    moe_gain,
    routes,
    route_weight,
    gate_weight,
    up_weight,
    down_weight,
):
    groups, ranks = lax.axis_size("ep"), lax.axis_size("tp")
    chips, total = ranks // 2, groups * ranks
    row_count, width = moe_rows.shape
    units = gate_weight.shape[2]
    chosen, weights = routes.T, route_weight.T
    named = chosen[:, None, :] == jnp.arange(groups, dtype=jnp.int32)[None, :, None]
    shares = jnp.sum(jnp.where(named, weights[:, None, :], 0.0), 0)
    tile_rows = -(-(groups + 1) // 8) * 8
    shares = jnp.pad(shares, ((0, tile_rows - groups), (0, 128 - row_count)))
    sinks = jnp.pad(
        sink_logits[None, :], ((groups, tile_rows - groups - 1), (0, 128 - sink_logits.shape[0]))
    )
    tile = shares + sinks
    bf16, f32 = jnp.bfloat16, jnp.float32
    vmem = pltpu.VMEM
    dma = pltpu.SemaphoreType.DMA
    sems = [(4,)]
    for count in (
        total,
        ranks,
        2,
        2 * chips,
        2 * chips,
        4 * chips,
        chips,
        2 * chips,
        chips,
        chips,
        chips,
        chips,
        chips,
        groups,
        2 * chips,
        chips,
        2 * chips,
        2 * chips,
    ):
        sems += [(count,), (count,)]
    block = (row_count, width)
    in_vmem = pl.BlockSpec(memory_space=pltpu.VMEM)
    in_any = pl.BlockSpec(memory_space=pl.ANY)
    return pl.pallas_call(
        functools.partial(fused_kernel, groups, ranks),
        out_shape=(
            jax.ShapeDtypeStruct((queries.shape[0] // ranks, width), bf16),
            jax.ShapeDtypeStruct(block, bf16),
        ),
        in_specs=[in_vmem] * 6 + [in_any] * 4,
        out_specs=(in_vmem, in_vmem),
        scratch_shapes=[
            vmem((groups, chips, 2) + block, bf16),
            vmem((groups, chips, 2) + block, bf16),
            vmem((groups, chips) + block, bf16),
            vmem((2, chips) + block, bf16),
            vmem((chips,) + block, bf16),
            vmem((chips,) + block, bf16),
            vmem((chips,) + block, bf16),
            vmem((ranks,) + out_weight.shape, bf16),
            vmem((ranks, WINDOW, 128), bf16),
            vmem((total, tile_rows, 128), f32),
            vmem((2, WINDOW, 128), bf16),
            vmem((2, 2 * WINDOW, 128), bf16),
            vmem((2, 2 * WINDOW, 128), bf16),
            vmem((WINDOW, ranks * 128), bf16),
            vmem((width, units), bf16),
            vmem((width, units), bf16),
            vmem((units, width), bf16),
        ]
        + [dma(shape) for shape in sems],
        compiler_params=pltpu.CompilerParams(
            collective_id=0, has_side_effects=True, vmem_limit_bytes=60 * 1024 * 1024
        ),
    )(
        queries,
        key_rows,
        value_rows,
        tile,
        moe_rows,
        moe_gain[None, :],
        out_weight,
        gate_weight,
        up_weight,
        down_weight,
    )


def body(
    queries,
    key_rows,
    value_rows,
    sink_logits,
    out_weight,
    moe_rows,
    moe_gain,
    routes,
    route_weight,
    gate_weight,
    up_weight,
    down_weight,
):
    groups, ranks = lax.axis_size("ep"), lax.axis_size("tp")
    fits = groups == 4 and ranks % 2 == 0 and ranks <= 8
    fits = fits and queries.shape == (ranks * WINDOW, 2 * HEAD_DIM)
    fits = fits and key_rows.shape[1] == 128 and moe_rows.shape[0] % 32 == 0
    if fits:
        return fused(
            queries,
            key_rows,
            value_rows,
            sink_logits,
            out_weight,
            moe_rows,
            moe_gain,
            routes,
            route_weight,
            gate_weight,
            up_weight,
            down_weight,
        )
    mixer_out = mixer(queries, key_rows, value_rows, sink_logits, out_weight)
    moe_out = experts(moe_rows, moe_gain, routes, route_weight, gate_weight, up_weight, down_weight)
    return (mixer_out, moe_out)


def solution(mesh):
    in_specs = (
        P("ep", "tp"),
        P("ep", None),
        P("ep", None),
        P("tp"),
        P("tp", None),
        P(("ep", "tp"), None),
        P(),
        P(("ep", "tp"), None),
        P(("ep", "tp"), None),
        P("ep", None, "tp"),
        P("ep", None, "tp"),
        P("ep", "tp", None),
    )
    out_specs = (P(("ep", "tp"), None), P(("ep", "tp"), None))
    return jax.shard_map(body, mesh=mesh, in_specs=in_specs, out_specs=out_specs, check_vma=False)
```
